256 devices in a mesh: vp: 16 (over y, x), dp: 16 (over z, core).
Axes of the slice: x: 4, y: 4, z: 8, core: 2. Of those that a mesh axis runs over, the one named last changes fastest.
Arguments:
- hidden_act: bfloat16 [8192, 8192], P('dp', 'vp'), may hold values from 0 to 36
- down_weight: bfloat16 [8192, 2048], P('vp'), may hold values from -0.0625 to 0.0625
- residual: bfloat16 [8192, 2048], P(('dp', 'vp')), may hold values from -300 to 300
- post_gain: float32 [2048], replicated, may hold values from 0.1 to 1.9
- final_gain: float32 [2048], replicated, may hold values from 0.1 to 1.9
- vocab: bfloat16 [2048, 32768], P(None, 'vp'), may hold values from -0.33 to 0.33
- vocab_bias: float32 [32768], P('vp'), may hold values from -2.5 to 2.5
- target_ids: int32 [8192, 4], P('dp'), may hold values from 0 to 32767
- target_weights: float32 [8192, 4], P('dp'), may hold values from 0 to 1, as said below
Outputs:
- losses: float32 [8192], P(('dp', 'vp'))
- stream_grad: float32 [8192, 2048], P(('dp', 'vp'))
- vocab_grad: float32 [2048, 32768], P('dp', 'vp')
The draws below stay inside these ranges and needn't reach their ends.
Inputs may be any that keep to these rules, and one draw needn't show every extreme that they name: `target_weights`: the 4 weights of a token add up to one.
All inputs are finite; a program needn't handle non-finite values.
Results may differ from the reference program's by a relative error of at most 0.01225.
Values may be sent and summed in bfloat16 or wider, within the bound.
No kernel may reach another device: no remote copies, remote signals or barrier semaphores. Data moves between devices by JAX's collectives and lax.ppermute only.
A program may use at most 128 MiB of HBM per device.

```python
import math
import jax
import jax.numpy as jnp
import numpy as np
from jax import lax

D = 2048
FF = 8192
V = 32768
TOPK = 4
TOK_GRP = 512
TOKENS = 8192
N_VP = 16
N_DP = 16


def spike_signs(key):
    return (jax.random.randint(jax.random.fold_in(key, 4242), (D,), 0, 2) * 2 - 1).astype(jnp.float32)


def draw_hidden_act(key, part):
    values = jax.random.normal(jax.random.fold_in(key, 41), (TOKENS, FF), jnp.float32)
    values = jnp.clip(values, -6.0, 6.0)
    positive = jnp.maximum(values, 0.0)
    return (positive * positive).astype(jnp.bfloat16)


def draw_residual(key, part):
    values = jnp.clip(jax.random.normal(jax.random.fold_in(key, 11), (TOKENS, D), jnp.float32), -6.0, 6.0)
    marked = (jnp.arange(TOKENS) % 61 == 3)[:, None]
    values = jnp.where(marked, 300.0 * spike_signs(key)[None, :], values)
    return values.astype(jnp.bfloat16)


def draw_vocab(key, part):
    values = 0.055 * jnp.clip(jax.random.normal(jax.random.fold_in(key, 21), (D, V), jnp.float32), -6.0, 6.0)
    marked = (jnp.arange(V) % 509 == 7)[None, :]
    values = jnp.where(marked, 256.0 / D * spike_signs(key)[:, None], values)
    return values.astype(jnp.bfloat16)


def draw_vocab_bias(key, part):
    offsets = jax.random.uniform(jax.random.fold_in(key, 31), (N_VP,), jnp.float32, -1.5, 1.5)
    shard_of = jnp.arange(V) // (V // N_VP)
    values = 0.5 * jnp.clip(jax.random.normal(jax.random.fold_in(key, 32), (V,), jnp.float32), -2.0, 2.0)
    return offsets[shard_of] + values


def draw_target_weights(key, part):
    logits = 1.5 * jax.random.normal(jax.random.fold_in(key, 52), (TOKENS, TOPK), jnp.float32)
    return jax.nn.softmax(logits, axis=-1)


def place_ends(entries, key, smallest, top_value):
    spot = [jax.random.randint(jax.random.fold_in(key, axis), (), 0, length) for axis, length in enumerate(entries.shape)]
    widest = entries.shape.index(max(entries.shape))
    next_to = spot[:widest] + [(spot[widest] + 1) % entries.shape[widest]] + spot[widest + 1:]
    return entries.at[tuple(spot)].set(smallest).at[tuple(next_to)].set(top_value)


def steps_of(own_key, extent, cuts, low, largest):
    factor_of = 1.0
    for axis_at, parts in cuts:
        draws = jax.random.uniform(jax.random.fold_in(jax.random.fold_in(own_key, 6), axis_at), (parts,), jnp.float32, low / len(cuts), largest / len(cuts))
        factor_of = factor_of * jnp.repeat(jnp.exp(draws), extent[axis_at] // parts).reshape((-1,) + (1,) * (len(extent) - 1 - axis_at))
    return factor_of


def rank_table(amount, slope):
    weights = [(1 << 20) // math.isqrt(standing ** slope) + 1 for standing in range(1, amount + 1)]
    scale = 1 + sum(weights) // (1 << 30)
    return np.cumsum(np.array([max(1, weight // scale) for weight in weights]))


def ranked_ids(stream_key, shape, count, slope):
    table = rank_table(count, slope)
    pick = jax.random.randint(jax.random.fold_in(stream_key, 1), shape, 0, int(table[count - 1]))
    standing = jnp.searchsorted(jnp.asarray(table, jnp.int32), pick, side="right")
    return jax.random.permutation(jax.random.fold_in(stream_key, 2), count)[standing].astype(jnp.int32)


def centred(key, dims, scale, reach, pieces=(), kind=jnp.bfloat16):
    values = scale * jax.random.normal(key, dims, jnp.float32)
    if pieces:
        values = values * steps_of(key, dims, pieces, -0.22, 0.18)
    return jnp.clip(values, -reach, reach).astype(kind)


def setup_inputs(seed: int = 0) -> dict:
    splits = jax.random.split(jax.random.key(seed), 10)
    hidden_act = draw_hidden_act(jax.random.fold_in(splits[9], 71), 0)
    down_weight = centred(splits[1], (FF, D), FF ** -0.5, 0.0625, ((0, 16),))
    residual = draw_residual(jax.random.fold_in(splits[9], 71), 0)
    post_gain = jnp.clip(1.0 + 0.18 * jax.random.normal(splits[3], (D,), jnp.float32), 0.1, 1.9)
    final_gain = jnp.clip(1.0 + 0.18 * jax.random.normal(splits[4], (D,), jnp.float32), 0.1, 1.9)
    vocab = draw_vocab(jax.random.fold_in(splits[9], 71), 0)
    vocab_bias = draw_vocab_bias(jax.random.fold_in(splits[9], 71), 0)
    target_ids = place_ends(ranked_ids(splits[7], (TOKENS, TOPK), V, 2), jax.random.fold_in(splits[7], 3), 0, V - 1).astype(jnp.int32)
    target_weights = draw_target_weights(jax.random.fold_in(splits[9], 71), 0)
    return dict(hidden_act=hidden_act, down_weight=down_weight, residual=residual, post_gain=post_gain, final_gain=final_gain, vocab=vocab, vocab_bias=vocab_bias, target_ids=target_ids, target_weights=target_weights)


epsilon = 1e-06
z_weight = 0.001
loss_scale = 32.0

def inverse_rms(values):
    return lax.rsqrt(lax.optimization_barrier(jnp.mean(values * values, axis=-1, keepdims=True)) + epsilon)

def reference(hidden_act, down_weight, residual, post_gain, final_gain, vocab, vocab_bias, target_ids, target_weights):
    branch = jnp.dot(hidden_act, down_weight, preferred_element_type=jnp.float32)
    stream = residual.astype(jnp.float32) + branch * inverse_rms(branch) * post_gain
    inverse = inverse_rms(stream)
    normed = (stream * inverse * final_gain).astype(jnp.bfloat16)
    columns = jnp.arange(V, dtype=jnp.int32)[None, :]

    def group(matrix_acc, inputs):
        row_block, target_block, weight_block = inputs
        scores = jnp.dot(row_block, vocab, preferred_element_type=jnp.float32) + vocab_bias
        row_max = lax.optimization_barrier(jnp.max(scores, axis=1))
        row_sum = lax.optimization_barrier(jnp.sum(jnp.exp(scores - row_max[:, None]), axis=1))
        log_norm = row_max + jnp.log(row_sum)
        wanted = jnp.zeros(scores.shape, jnp.float32)
        for target_k in range(TOPK):
            wanted = wanted + jnp.where(target_block[:, target_k:target_k + 1] == columns, weight_block[:, target_k:target_k + 1], 0.0)
        target_score = lax.optimization_barrier(jnp.sum(wanted * scores, axis=1))
        losses = log_norm - target_score + z_weight * log_norm * log_norm
        probability = jnp.exp(scores - log_norm[:, None])
        score_grads = (loss_scale * (probability * (1.0 + 2.0 * z_weight * log_norm)[:, None] - wanted)).astype(jnp.bfloat16)
        row_grad = lax.dot_general(score_grads, vocab, (((1,), (1,)), ((), ())), preferred_element_type=jnp.float32)
        matrix_acc = matrix_acc + lax.dot_general(row_block, score_grads, (((0,), (0,)), ((), ())), preferred_element_type=jnp.float32)
        return (matrix_acc, (losses, row_grad))
    stacked = (normed.reshape(N_DP, TOK_GRP, D), target_ids.reshape(N_DP, TOK_GRP, TOPK), target_weights.reshape(N_DP, TOK_GRP, TOPK))
    vocab_grad, outputs = lax.scan(group, jnp.zeros((D, V), jnp.float32), stacked)
    losses = outputs[0].reshape(TOKENS)
    row_grad = outputs[1].reshape(TOKENS, D)
    upstream = row_grad * final_gain
    stream_grad = inverse * (upstream - stream * inverse * inverse * lax.optimization_barrier(jnp.mean(upstream * stream, axis=-1, keepdims=True)))
    return (losses, stream_grad, vocab_grad)
```

```python
import jax
import jax.numpy as jnp
from jax import lax
from jax.sharding import Mesh
from jax.sharding import PartitionSpec as P


F32 = jnp.float32
BF16 = jnp.bfloat16
VP = ("y", "x")
DP = ("z", "c")
DP_VP = ("z", "c", "y", "x")

epsilon = 1e-06
z_weight = 0.001
loss_scale = 32.0


def exchange(parts, axis):
    return lax.all_to_all(parts, axis, split_axis=0, concat_axis=0, tiled=True)


def summed_over(rows, axis):
    size = lax.axis_size(axis)
    parts = rows.astype(BF16).reshape(size, rows.shape[0] // size, rows.shape[1])
    return jnp.sum(exchange(parts, axis).astype(F32), axis=0)


def copied_over(rows, axis):
    size = lax.axis_size(axis)
    copies = jnp.broadcast_to(rows, (size, *rows.shape))
    return exchange(copies, axis).reshape(size * rows.shape[0], rows.shape[1])


def two_halves(x):
    ny, nx = lax.axis_size("y"), lax.axis_size("x")
    part = x.shape[0] // (ny * nx * 2)
    split = x.reshape(ny, nx, 2, part, *x.shape[1:])
    first = jnp.swapaxes(split[:, :, 0], 0, 1).reshape(x.shape[0] // 2, *x.shape[1:])
    second = split[:, :, 1].reshape(x.shape[0] // 2, *x.shape[1:])
    return first, second


def inverse_rms(values):
    return lax.rsqrt(jnp.mean(values * values, axis=-1, keepdims=True) + epsilon)


def shards(
    hidden_act,
    down_weight,
    residual,
    post_gain,
    final_gain,
    vocab,
    vocab_bias,
    target_ids,
    target_weights,
):
    own_rows = residual.shape[0]
    half_rows = own_rows // 2
    width, columns = vocab.shape
    vp_index = lax.axis_index(VP)
    z_index = lax.axis_index("z")
    core = lax.axis_index("c")
    n_z = lax.axis_size("z")
    n_c = lax.axis_size("c")

    act_a, act_b = two_halves(hidden_act)
    sum_a = summed_over(jnp.dot(act_a, down_weight, preferred_element_type=F32), "x")
    sum_b = summed_over(jnp.dot(act_b, down_weight, preferred_element_type=F32), "y")
    branch = jnp.concatenate([summed_over(sum_a, "y"), summed_over(sum_b, "x")])
    stream = residual.astype(F32) + branch * inverse_rms(branch) * post_gain
    inverse = inverse_rms(stream)
    normed = (stream * inverse * final_gain).astype(BF16)

    rows_a = copied_over(copied_over(normed[:half_rows], "y"), "x")
    rows_b = copied_over(copied_over(normed[half_rows:], "x"), "y")
    gathered = jnp.concatenate([rows_a, rows_b])
    ids = jnp.concatenate(two_halves(target_ids)) - vp_index * columns
    weights = jnp.concatenate(two_halves(target_weights))
    position = lax.broadcasted_iota(jnp.int32, (1, columns), 1)

    def wanted():
        found = jnp.zeros((gathered.shape[0], columns), F32)
        for k in range(ids.shape[1]):
            found = found + jnp.where(ids[:, k : k + 1] == position, weights[:, k : k + 1], 0.0)
        return found

    scores = jnp.dot(gathered, vocab, preferred_element_type=F32) + vocab_bias
    local_max = jnp.max(scores, axis=1)
    powers = jnp.exp(scores - local_max[:, None])
    local_sum = jnp.sum(powers, axis=1)
    local_target = jnp.sum(wanted() * scores, axis=1)
    n_vp = lax.axis_size(VP)
    stats = jnp.stack([local_max, local_sum, local_target])
    stats = exchange(jnp.broadcast_to(stats, (n_vp, *stats.shape)), VP)
    row_max = jnp.max(stats[:, 0], axis=0)
    row_sum = jnp.sum(stats[:, 1] * jnp.exp(stats[:, 0] - row_max), axis=0)
    target_score = jnp.sum(stats[:, 2], axis=0)
    log_norm = row_max + jnp.log(row_sum)
    group_losses = log_norm - target_score + z_weight * log_norm * log_norm
    y_index, x_index = lax.axis_index("y"), lax.axis_index("x")
    n_y, n_x = lax.axis_size("y"), lax.axis_size("x")
    half_group = group_losses.shape[0] // 2
    losses = jnp.concatenate(
        [
            lax.dynamic_slice_in_dim(group_losses, (x_index * n_y + y_index) * half_rows, half_rows),
            lax.dynamic_slice_in_dim(
                group_losses, half_group + (y_index * n_x + x_index) * half_rows, half_rows
            ),
        ]
    )
    scale = (jnp.exp(local_max - log_norm) * (1.0 + 2.0 * z_weight * log_norm))[:, None]
    grads = (loss_scale * (powers * scale - wanted())).astype(BF16)

    slice_rows = width // (n_z * n_c)
    turned = gathered.T
    half_columns = columns // 2

    def partial(distances, of_core, side):
        rows = [
            lax.dynamic_slice_in_dim(
                turned, (((z_index + dz) % n_z) * n_c + of_core) * slice_rows, slice_rows
            )
            for dz in distances
        ]
        rows = rows[0] if len(rows) == 1 else jnp.concatenate(rows)
        cols = grads[:, side * half_columns : (side + 1) * half_columns]
        return jnp.dot(rows, cols, preferred_element_type=F32)

    def swapped(x):
        return lax.ppermute(x, "c", [(0, 1), (1, 0)])

    far = n_z // 2
    chunk = {}
    for group in ([far], [far - 1, 1 - far], [k for d in range(far - 2, 0, -1) for k in (d, -d)] + [0]):
        for side in (0, 1):
            other = swapped(partial(group, 1 - core, side).astype(BF16))
            own = partial(group, core, side)
            both = own + other.astype(F32)
            for k, dz in enumerate(group):
                chunk[dz, side] = both[k * slice_rows : (k + 1) * slice_rows]

    total = [chunk[0, 0], chunk[0, 1]]
    for step, first_side in ((1, 0), (-1, 1)):
        ring = [(k, (k + step) % n_z) for k in range(n_z)]
        for side in (first_side, 1 - first_side):
            start = far if side == first_side else far - 1
            carried = None
            for distance in range(start, 0, -1):
                dz = distance * step if distance != far else far
                piece = chunk[dz, side]
                piece = piece if carried is None else piece + carried.astype(F32)
                carried = lax.ppermute(piece.astype(BF16), "z", ring)
            total[side] = total[side] + carried.astype(F32)
    vocab_grad = jnp.concatenate(total, axis=1)

    row_parts = lax.dot_general(
        grads, vocab, (((1,), (1,)), ((), ())), preferred_element_type=F32
    )
    part_a = summed_over(row_parts[:half_group], "x")
    part_b = summed_over(row_parts[half_group:], "y")
    row_grad = jnp.concatenate([summed_over(part_a, "y"), summed_over(part_b, "x")])
    upstream = row_grad * final_gain
    stream_grad = inverse * (
        upstream - stream * inverse * inverse * jnp.mean(upstream * stream, axis=-1, keepdims=True)
    )
    return (losses, stream_grad, vocab_grad)


def solution(mesh):
    split = Mesh(mesh.devices.reshape(4, 4, mesh.shape["dp"] // 2, 2), ("y", "x", "z", "c"))
    placed = (
        P(DP, VP),
        P(VP, None),
        P(DP_VP, None),
        P(),
        P(),
        P(None, VP),
        P(VP),
        P(DP, None),
        P(DP, None),
    )
    return jax.shard_map(
        shards,
        mesh=split,
        in_specs=placed,
        out_specs=(P(DP_VP), P(DP_VP, None), P(DP, VP)),
        check_vma=False,
    )
```

```python
import jax
import jax.numpy as jnp
from jax import lax
from jax.experimental import pallas as pl
from jax.experimental.pallas import tpu as pltpu
from jax.sharding import Mesh
from jax.sharding import PartitionSpec as P


F32 = jnp.float32
BF16 = jnp.bfloat16
VP = ("y", "x")
DP = ("z", "c")
DP_VP = ("z", "c", "y", "x")

epsilon = 1e-06
z_weight = 0.001
loss_scale = 32.0


def exchange(parts, axis):
    return lax.all_to_all(parts, axis, split_axis=0, concat_axis=0, tiled=True)


def summed_over(rows, axis):
    size = lax.axis_size(axis)
    parts = rows.astype(BF16).reshape(size, rows.shape[0] // size, rows.shape[1])
    return jnp.sum(exchange(parts, axis).astype(F32), axis=0)


def copied_over(rows, axis):
    size = lax.axis_size(axis)
    copies = jnp.broadcast_to(rows, (size, *rows.shape))
    return exchange(copies, axis).reshape(size * rows.shape[0], rows.shape[1])


def inverse_rms(values):
    return lax.rsqrt(jnp.mean(values * values, axis=-1, keepdims=True) + epsilon)


def call(kernel, grid, in_specs, out_specs, out_shape, operands, flops, after=(), scratch=(), scalars=None):
    lead = 0 if scalars is None else 1
    used = len(operands)

    def body(*refs):
        kernel(*refs[: lead + used], *refs[lead + used + len(after) :])

    moved = sum(x.size * x.dtype.itemsize for x in operands)
    return pl.pallas_call(
        body,
        grid_spec=pltpu.PrefetchScalarGridSpec(
            num_scalar_prefetch=lead,
            grid=grid,
            in_specs=list(in_specs) + [pl.BlockSpec(memory_space=pl.ANY)] * len(after),
            out_specs=out_specs,
            scratch_shapes=scratch,
        ),
        out_shape=out_shape,
        cost_estimate=pl.CostEstimate(flops=flops, bytes_accessed=moved, transcendentals=0),
    )(*(() if scalars is None else (scalars,)), *operands, *after)


LANES = 128
SCORE_BLOCK = 512


def wanted_matrix(ids, weights, columns, after):
    tokens = ids.shape[0]
    rows = 128

    def kernel(ids_ref, weights_ref, out_ref):
        wide = (rows, LANES)
        at_ids = [jnp.broadcast_to(ids_ref[:, k : k + 1], wide) for k in range(ids.shape[1])]
        at_weights = [jnp.broadcast_to(weights_ref[:, k : k + 1], wide) for k in range(ids.shape[1])]
        lane = lax.broadcasted_iota(jnp.int32, wide, 1)
        for at in range(0, columns, LANES):
            found = jnp.zeros(wide, F32)
            for k in range(ids.shape[1]):
                found = found + jnp.where(at_ids[k] == lane + at, at_weights[k], 0.0)
            out_ref[:, at : at + LANES] = found

    def block(shape):
        return pl.BlockSpec((rows, shape[1]), lambda i: (i, 0))

    return call(
        kernel,
        (tokens // rows,),
        [block(ids.shape), block(weights.shape)],
        block((tokens, columns)),
        jax.ShapeDtypeStruct((tokens, columns), F32),
        [ids, weights],
        8000 * tokens * columns // 1000,
        after,
    )


def turned(x, after):
    rows = 256

    def kernel(x_ref, out_ref):
        out_ref[...] = x_ref[...].T

    return call(
        kernel,
        (x.shape[0] // rows,),
        [pl.BlockSpec((rows, x.shape[1]), lambda i: (i, 0))],
        pl.BlockSpec((x.shape[1], rows), lambda i: (0, i)),
        jax.ShapeDtypeStruct(x.shape[::-1], x.dtype),
        [x],
        2000 * x.size,
        after,
    )


HBM = pl.BlockSpec(memory_space=pl.ANY)


def scored(rows, vocab, bias, wanted):
    tokens, width = rows.shape
    columns = vocab.shape[1]
    blocks = columns // SCORE_BLOCK

    def kernel(rows_hbm, vocab_hbm, bias_ref, wanted_hbm, scores_hbm, stats_ref, rows_in, vocab_in, wanted_in, out, sems):
        def across(j):
            return pl.ds(j * SCORE_BLOCK, SCORE_BLOCK)

        load_rows = pltpu.make_async_copy(rows_hbm, rows_in, sems.at[3, 0])
        load_vocab = [
            pltpu.make_async_copy(vocab_hbm.at[:, across(j)], vocab_in.at[j], sems.at[0, j])
            for j in range(blocks)
        ]
        load_wanted = [
            pltpu.make_async_copy(wanted_hbm.at[:, across(j)], wanted_in.at[j], sems.at[1, j])
            for j in range(blocks)
        ]
        store = [
            pltpu.make_async_copy(out.at[j], scores_hbm.at[:, across(j)], sems.at[2, j])
            for j in range(blocks)
        ]
        load_rows.start()
        for j in range(blocks):
            load_vocab[j].start()
            load_wanted[j].start()
        load_rows.wait()
        top = jnp.full((tokens, LANES), -jnp.inf, F32)
        total = jnp.zeros((tokens, LANES), F32)
        target = jnp.zeros((tokens, LANES), F32)
        for j in range(blocks):
            load_vocab[j].wait()
            out[j] = (
                jnp.dot(rows_in[...], vocab_in[j], preferred_element_type=F32)
                + bias_ref[:, j * SCORE_BLOCK : (j + 1) * SCORE_BLOCK]
            )
            store[j].start()
            load_wanted[j].wait()
            parts = [out[j, :, at : at + LANES] for at in range(0, SCORE_BLOCK, LANES)]
            new_top = top
            for part in parts:
                new_top = jnp.maximum(new_top, part)
            total = total * jnp.exp(top - new_top)
            for at, part in enumerate(parts):
                total = total + jnp.exp(part - new_top)
                target = target + wanted_in[j, :, at * LANES : (at + 1) * LANES] * part
            top = new_top
        row_top = jnp.max(top, axis=1, keepdims=True)
        row_total = jnp.sum(total * jnp.exp(top - row_top), axis=1, keepdims=True)
        row_target = jnp.sum(target, axis=1, keepdims=True)
        lane = lax.broadcasted_iota(jnp.int32, (tokens, LANES), 1)
        packed = jnp.where(lane == 0, row_top, jnp.where(lane == 1, row_total, row_target))
        stats_ref[...] = packed.T[:8]
        for copy in store:
            copy.wait()

    scores, stats = call(
        kernel,
        (1,),
        [HBM, HBM, pl.BlockSpec((1, columns), lambda i: (0, 0)), HBM],
        [HBM, pl.BlockSpec((8, tokens), lambda i: (0, 0))],
        [
            jax.ShapeDtypeStruct((tokens, columns), F32),
            jax.ShapeDtypeStruct((8, tokens), F32),
        ],
        [rows, vocab, bias.reshape(1, columns), wanted],
        2 * tokens * width * columns,
        scratch=[
            pltpu.VMEM((tokens, width), BF16),
            pltpu.VMEM((blocks, width, SCORE_BLOCK), BF16),
            pltpu.VMEM((blocks, tokens, SCORE_BLOCK), F32),
            pltpu.VMEM((blocks, tokens, SCORE_BLOCK), F32),
            pltpu.SemaphoreType.DMA((4, blocks)),
        ],
    )
    return scores, stats[:3]


def gradients(scores, log_norm, wanted, rows, index, lists, chunk):
    tokens, columns = scores.shape
    width = rows.shape[0]
    half = columns // 2
    part = 128
    steps = tokens // part
    tall = 512
    count = sum(len(some) for some in lists)

    def kernel(index_ref, scores_hbm, norm_ref, wanted_hbm, rows_hbm, grads_hbm, *refs):
        outs = refs[: len(lists)]
        scores_in, wanted_in, rows_in, kept, product, load_sems, store_sems, out_sems = refs[len(lists) :]

        def down(i):
            return pl.ds(i * part, part)

        load_scores = [
            pltpu.make_async_copy(scores_hbm.at[down(i)], scores_in.at[down(i)], load_sems.at[0, i])
            for i in range(steps)
        ]
        load_wanted = [
            pltpu.make_async_copy(wanted_hbm.at[down(i)], wanted_in.at[down(i)], load_sems.at[1, i])
            for i in range(steps)
        ]
        load_rows = pltpu.make_async_copy(rows_hbm, rows_in, load_sems.at[2, 0])
        for i in range(steps):
            load_scores[i].start()
            load_wanted[i].start()
        load_rows.start()
        store_grads = []
        for i in range(steps):
            load_scores[i].wait()
            load_wanted[i].wait()
            norm = jnp.broadcast_to(norm_ref[i * part : (i + 1) * part], (part, LANES))
            factor = 1.0 + 2.0 * z_weight * norm
            for at in range(0, columns, LANES):
                cell = (slice(i * part, (i + 1) * part), slice(at, at + LANES))
                probability = jnp.exp(scores_in[cell] - norm)
                value = (loss_scale * (probability * factor - wanted_in[cell])).astype(BF16)
                kept[at // half, cell[0], at % half : at % half + LANES] = value
            for side in (0, 1):
                store_grads.append(
                    pltpu.make_async_copy(
                        kept.at[side, down(i)],
                        grads_hbm.at[down(i), pl.ds(side * half, half)],
                        store_sems.at[side, i],
                    )
                )
                store_grads[-1].start()
        load_rows.wait()
        store_blocks = []
        for slot in (0, 1):
            side = index_ref[0] if slot == 0 else 1 - index_ref[0]
            for at in range(0, width, tall):
                product[slot, at : at + tall] = jnp.dot(
                    rows_in[at : at + tall], kept[side], preferred_element_type=F32
                ).astype(BF16)
            flat = 0
            for out, some in zip(outs, lists):
                for k, (place, its_slot) in enumerate(some):
                    if its_slot == slot:
                        start = pl.multiple_of(index_ref[place] * chunk, chunk)
                        store_blocks.append(
                            pltpu.make_async_copy(
                                product.at[slot, pl.ds(start, chunk)], out.at[k], out_sems.at[flat]
                            )
                        )
                        store_blocks[-1].start()
                    flat += 1
        for copy in store_grads + store_blocks:
            copy.wait()

    results = call(
        kernel,
        (1,),
        [HBM, pl.BlockSpec((tokens, 1), lambda i, idx: (0, 0)), HBM, HBM],
        [HBM] * (1 + len(lists)),
        [jax.ShapeDtypeStruct(scores.shape, BF16)]
        + [jax.ShapeDtypeStruct((len(some), chunk, half), BF16) for some in lists],
        [scores, log_norm[:, None], wanted, rows],
        2 * width * columns * tokens,
        scratch=[
            pltpu.VMEM((tokens, columns), F32),
            pltpu.VMEM((tokens, columns), F32),
            pltpu.VMEM(rows.shape, BF16),
            pltpu.VMEM((2, tokens, half), BF16),
            pltpu.VMEM((2, width, half), BF16),
            pltpu.SemaphoreType.DMA((3, steps)),
            pltpu.SemaphoreType.DMA((2, steps)),
            pltpu.SemaphoreType.DMA((count,)),
        ],
        scalars=index,
    )
    return results[0], results[1:]


def row_gradients(grads, vocab):
    tokens, columns = grads.shape
    width = vocab.shape[0]
    blocks = 4
    rows = width // blocks

    def kernel(grads_hbm, vocab_hbm, out_hbm, grads_in, vocab_in, out, sems):
        load_grads = pltpu.make_async_copy(grads_hbm, grads_in, sems.at[2, 0])
        load_vocab = [
            pltpu.make_async_copy(vocab_hbm.at[pl.ds(j * rows, rows)], vocab_in.at[j], sems.at[0, j])
            for j in range(blocks)
        ]
        store = [
            pltpu.make_async_copy(out.at[j], out_hbm.at[:, pl.ds(j * rows, rows)], sems.at[1, j])
            for j in range(blocks)
        ]
        load_grads.start()
        for copy in load_vocab:
            copy.start()
        load_grads.wait()
        for j in range(blocks):
            load_vocab[j].wait()
            out[j] = lax.dot_general(
                grads_in[...], vocab_in[j], (((1,), (1,)), ((), ())), preferred_element_type=F32
            ).astype(BF16)
            store[j].start()
        for copy in store:
            copy.wait()

    return call(
        kernel,
        (1,),
        [HBM, HBM],
        HBM,
        jax.ShapeDtypeStruct((tokens, width), BF16),
        [grads, vocab],
        2 * tokens * columns * width,
        scratch=[
            pltpu.VMEM((tokens, columns), BF16),
            pltpu.VMEM((blocks, rows, columns), BF16),
            pltpu.VMEM((blocks, tokens, rows), BF16),
            pltpu.SemaphoreType.DMA((3, blocks)),
        ],
    )


def shards(
    hidden_act,
    down_weight,
    residual,
    post_gain,
    final_gain,
    vocab,
    vocab_bias,
    target_ids,
    target_weights,
):
    own_rows = residual.shape[0]
    width, columns = vocab.shape
    vp_index = lax.axis_index(VP)
    z_index = lax.axis_index("z")
    core = lax.axis_index("c")
    n_z = lax.axis_size("z")

    branch_parts = jnp.dot(hidden_act, down_weight, preferred_element_type=F32).astype(BF16)
    branch = summed_over(branch_parts, VP)
    stream = residual.astype(F32) + branch * inverse_rms(branch) * post_gain
    inverse = inverse_rms(stream)
    normed = (stream * inverse * final_gain).astype(BF16)

    gathered = copied_over(normed, VP)
    ids = target_ids - vp_index * columns
    wanted = wanted_matrix(ids, target_weights, columns, (branch_parts,))
    scores, stats = scored(gathered, vocab, vocab_bias, wanted)
    normed_rows = turned(gathered, (stats,))
    n_vp = lax.axis_size(VP)
    stats = exchange(jnp.broadcast_to(stats, (n_vp, *stats.shape)), VP)
    row_max = jnp.max(stats[:, 0], axis=0)
    row_sum = jnp.sum(stats[:, 1] * jnp.exp(stats[:, 0] - row_max), axis=0)
    target_score = jnp.sum(stats[:, 2], axis=0)
    log_norm = row_max + jnp.log(row_sum)
    group_losses = log_norm - target_score + z_weight * log_norm * log_norm
    losses = lax.dynamic_slice_in_dim(group_losses, vp_index * own_rows, own_rows)
    chunk = width // n_z
    far = n_z // 2
    way = 1 - 2 * core

    def swapped(x):
        return lax.ppermute(x, "c", [(0, 1), (1, 0)])

    ring = [
        (z * 2 + c, (z + (1, -1)[c]) % n_z * 2 + c) for z in range(n_z) for c in (0, 1)
    ]

    def sent(x):
        return lax.ppermute(x.astype(BF16), DP, ring)

    index = jnp.stack(
        [1 - core]
        + [(z_index + way * d + n_z) % n_z for d in range(far + 1)]
        + [(z_index - way * d + n_z) % n_z for d in range(far + 1)]
    )

    def own_block(distance, lane):
        return (1 + distance, 1 - lane)

    def their_block(distance, lane):
        return (2 + far + distance, lane)

    first = [(far, 0), (far - 1, 1), (far - 1, 0)]
    rest = [(d, lane) for d in range(far - 2, 0, -1) for lane in (1, 0)]
    owned = first + rest + [(0, 0), (0, 1)]
    grads, products = gradients(
        scores,
        log_norm,
        wanted,
        normed_rows,
        index,
        [[their_block(*key) for key in first]]
        + [[their_block(*key)] for key in rest]
        + [[own_block(*key)] for key in owned],
        chunk,
    )
    passed_first = swapped(products[0])
    passed = {key: passed_first[at] for at, key in enumerate(first)}
    passed.update({key: swapped(block)[0] for key, block in zip(rest, products[1:])})
    own = {key: block[0] for key, block in zip(owned, products[1 + len(rest) :])}

    def message(key, *carried):
        return sum(x.astype(F32) for x in (own[key], passed[key], *carried)).astype(BF16)

    carried = [sent(message((far, 0))), sent(message((far - 1, 1)))]
    for distance in range(far - 1, 0, -1):
        for lane, key in ((0, (distance, 0)), (1, (distance - 1, 1))):
            if key in owned and key[0] > 0:
                carried[lane] = sent(message(key, carried[lane]))
    slice_rows = chunk // 2
    arrived, passed = [], []
    for lane in (0, 1):
        whole = own[0, lane].astype(F32) + carried[lane].astype(F32)
        arrived.append(lax.dynamic_slice_in_dim(whole, core * slice_rows, slice_rows))
        theirs = lax.dynamic_slice_in_dim(whole, (1 - core) * slice_rows, slice_rows)
        passed.append(swapped(theirs.astype(BF16)).astype(F32))
    lanes = [arrived[0] + passed[1], arrived[1] + passed[0]]
    vocab_grad = jnp.concatenate(
        [jnp.where(core == 0, lanes[0], lanes[1]), jnp.where(core == 0, lanes[1], lanes[0])], axis=1
    )

    row_parts = row_gradients(grads, vocab)
    row_grad = summed_over(row_parts, VP)
    upstream = row_grad * final_gain
    stream_grad = inverse * (
        upstream - stream * inverse * inverse * jnp.mean(upstream * stream, axis=-1, keepdims=True)
    )
    return (losses, stream_grad, vocab_grad)


def solution(mesh):
    split = Mesh(mesh.devices.reshape(4, 4, mesh.shape["dp"] // 2, 2), ("y", "x", "z", "c"))
    placed = (
        P(DP, VP),
        P(VP, None),
        P(DP_VP, None),
        P(),
        P(),
        P(None, VP),
        P(VP),
        P(DP, None),
        P(DP, None),
    )

    return jax.shard_map(
        shards,
        mesh=split,
        in_specs=placed,
        out_specs=(P(DP_VP), P(DP_VP, None), P(DP, VP)),
        check_vma=False,
    )
```

```python
import jax
import jax.numpy as jnp
from jax import lax
from jax.experimental import pallas as pl
from jax.experimental.pallas import tpu as pltpu
from jax.sharding import Mesh
from jax.sharding import PartitionSpec as P


F32 = jnp.float32
BF16 = jnp.bfloat16
VP = ("y", "x")
DP = ("z", "c")
DP_VP = ("z", "c", "y", "x")

epsilon = 1e-06
z_weight = 0.001
loss_scale = 32.0


def exchange(parts, axis):
    return lax.all_to_all(parts, axis, split_axis=0, concat_axis=0, tiled=True)


def summed_over(rows, axis):
    size = lax.axis_size(axis)
    parts = rows.astype(BF16).reshape(size, rows.shape[0] // size, rows.shape[1])
    return jnp.sum(exchange(parts, axis).astype(F32), axis=0)


def copied_over(rows, axis):
    size = lax.axis_size(axis)
    copies = jnp.broadcast_to(rows, (size, *rows.shape))
    return exchange(copies, axis).reshape(size * rows.shape[0], rows.shape[1])


def inverse_rms(values):
    return lax.rsqrt(jnp.mean(values * values, axis=-1, keepdims=True) + epsilon)


def call(kernel, grid, in_specs, out_specs, out_shape, operands, flops, after=(), scratch=(), scalars=None, aliases={}, vmem=16):
    lead = 0 if scalars is None else 1
    used = len(operands)

    def body(*refs):
        kernel(*refs[: lead + used], *refs[lead + used + len(after) :])

    moved = sum(x.size * x.dtype.itemsize for x in operands)
    return pl.pallas_call(
        body,
        grid_spec=pltpu.PrefetchScalarGridSpec(
            num_scalar_prefetch=lead,
            grid=grid,
            in_specs=list(in_specs) + [pl.BlockSpec(memory_space=pl.ANY)] * len(after),
            out_specs=out_specs,
            scratch_shapes=scratch,
        ),
        out_shape=out_shape,
        input_output_aliases=aliases,
        compiler_params=pltpu.CompilerParams(vmem_limit_bytes=vmem << 20),
        cost_estimate=pl.CostEstimate(flops=flops, bytes_accessed=moved, transcendentals=0),
    )(*(() if scalars is None else (scalars,)), *operands, *after)


LANES = 128
SCORE_BLOCK = 512
HBM = pl.BlockSpec(memory_space=pltpu.HBM)
NEAR = pl.BlockSpec(memory_space=pltpu.VMEM)


def wanted_matrix(ids, weights, columns, after):
    tokens = ids.shape[0]
    rows = 128

    def kernel(ids_ref, weights_ref, out_ref):
        wide = (rows, LANES)
        at_ids = [jnp.broadcast_to(ids_ref[:, k : k + 1], wide) for k in range(ids.shape[1])]
        at_weights = [jnp.broadcast_to(weights_ref[:, k : k + 1], wide) for k in range(ids.shape[1])]
        lane = lax.broadcasted_iota(jnp.int32, wide, 1)
        for at in range(0, columns, LANES):
            found = jnp.zeros(wide, F32)
            for k in range(ids.shape[1]):
                found = found + jnp.where(at_ids[k] == lane + at, at_weights[k], 0.0)
            out_ref[:, at : at + LANES] = found

    def block(shape):
        return pl.BlockSpec((rows, shape[1]), lambda i: (i, 0))

    return call(
        kernel,
        (tokens // rows,),
        [block(ids.shape), block(weights.shape)],
        block((tokens, columns)),
        jax.ShapeDtypeStruct((tokens, columns), F32),
        [ids, weights],
        8 * tokens * columns,
        after,
    )


def scored(rows, vocab, bias, wanted):
    tokens, width = rows.shape
    columns = vocab.shape[1]
    blocks = [slice(at, at + SCORE_BLOCK) for at in range(0, columns, SCORE_BLOCK)]

    def kernel(rows_ref, vocab_hbm, bias_ref, wanted_hbm, out_ref, stats_ref, vocab_ref, wanted_ref, turned_ref, sems):
        deep = width // 4
        load_vocab = [
            pltpu.make_async_copy(
                vocab_hbm.at[pl.ds(i * deep, deep)], vocab_ref.at[pl.ds(i * deep, deep)], sems.at[i]
            )
            for i in range(4)
        ]
        load_wanted = pltpu.make_async_copy(wanted_hbm, wanted_ref, sems.at[4])
        near, rest = slice(0, 2 * deep), slice(2 * deep, width)
        load_vocab[0].start()
        load_vocab[1].start()
        load_vocab[0].wait()
        load_vocab[2].start()
        load_vocab[1].wait()
        load_vocab[3].start()
        load_wanted.start()
        turn = width // len(blocks)
        for j, across in enumerate(blocks):
            out_ref[:, across] = jnp.dot(
                rows_ref[:, near], vocab_ref[near, across], preferred_element_type=F32
            )
            turned_ref[j * turn : (j + 1) * turn] = rows_ref[:, j * turn : (j + 1) * turn].T
        top = jnp.full((tokens, LANES), -jnp.inf, F32)
        total = jnp.zeros((tokens, LANES), F32)
        target = jnp.zeros((tokens, LANES), F32)
        load_vocab[2].wait()
        load_vocab[3].wait()
        load_wanted.wait()
        for j in range(len(blocks) + 1):
            if j < len(blocks):
                across = blocks[j]
                out_ref[:, across] = (
                    out_ref[:, across]
                    + jnp.dot(rows_ref[:, rest], vocab_ref[rest, across], preferred_element_type=F32)
                    + bias_ref[:, across]
                )
            if j > 0:
                across = blocks[j - 1]
                lanes = [slice(at, at + LANES) for at in range(across.start, across.stop, LANES)]
                new_top = top
                for at in lanes:
                    new_top = jnp.maximum(new_top, out_ref[:, at])
                total = total * jnp.exp(top - new_top)
                for at in lanes:
                    part = out_ref[:, at]
                    total = total + jnp.exp(part - new_top)
                    target = target + wanted_ref[:, at] * part
                top = new_top
        row_top = jnp.max(top, axis=1, keepdims=True)
        row_total = jnp.sum(total * jnp.exp(top - row_top), axis=1, keepdims=True)
        row_target = jnp.sum(target, axis=1, keepdims=True)
        lane = lax.broadcasted_iota(jnp.int32, (tokens, LANES), 1)
        packed = jnp.where(lane == 0, row_top, jnp.where(lane == 1, row_total, row_target))
        stats_ref[...] = packed.T[:8]

    scores, stats, near_vocab, near_wanted, turned = call(
        kernel,
        (1,),
        [NEAR, HBM, pl.BlockSpec((1, columns), lambda i: (0, 0)), HBM],
        [NEAR, pl.BlockSpec((8, tokens), lambda i: (0, 0)), NEAR, NEAR, NEAR],
        [
            pltpu.VMEM((tokens, columns), F32),
            jax.ShapeDtypeStruct((8, tokens), F32),
            pltpu.VMEM(vocab.shape, vocab.dtype),
            pltpu.VMEM(wanted.shape, wanted.dtype),
            pltpu.VMEM((width, tokens), rows.dtype),
        ],
        [rows, vocab, bias.reshape(1, columns), wanted],
        2 * tokens * width * columns,
        scratch=[pltpu.SemaphoreType.DMA((5,))],
        vmem=42,
    )
    return scores, stats[:3], near_vocab, near_wanted, turned


def gradients(scores, log_norm, wanted, rows, index, lists, chunk):
    tokens, columns = scores.shape
    width = rows.shape[0]
    half = columns // 2
    part = 128

    def kernel(index_ref, scores_ref, norm_ref, wanted_ref, rows_ref, grads_ref, *refs):
        outs, kept = refs[:-1], refs[-1]
        norms = jnp.broadcast_to(norm_ref[...], (LANES, tokens)).T
        for i in range(0, tokens, part):
            norm = norms[i : i + part]
            factor = 1.0 + 2.0 * z_weight * norm
            for at in range(0, columns, LANES):
                cell = (slice(i, i + part), slice(at, at + LANES))
                probability = jnp.exp(scores_ref[cell] - norm)
                value = (loss_scale * (probability * factor - wanted_ref[cell])).astype(BF16)
                grads_ref[cell] = value
                kept[at // half, cell[0], at % half : at % half + LANES] = value
        for out, some in zip(outs, lists):
            for k, (place, slot) in enumerate(some):
                side = index_ref[0] if slot == 0 else 1 - index_ref[0]
                start = pl.multiple_of(index_ref[place] * chunk, chunk)
                out[k] = jnp.dot(
                    rows_ref[pl.ds(start, chunk)], kept[side], preferred_element_type=F32
                ).astype(BF16)

    results = call(
        kernel,
        (1,),
        [NEAR, pl.BlockSpec((1, tokens), lambda i, idx: (0, 0)), NEAR, NEAR],
        [NEAR] * (1 + len(lists)),
        [pltpu.VMEM(scores.shape, BF16)]
        + [pltpu.VMEM((len(some), chunk, half), BF16) for some in lists],
        [scores, log_norm[None], wanted, rows],
        2 * width * columns * tokens,
        scratch=[pltpu.VMEM((2, tokens, half), BF16)],
        scalars=index,
    )
    return results[0], results[1:]


def row_gradients(grads, vocab):
    tokens, columns = grads.shape
    width = vocab.shape[0]

    def kernel(grads_ref, vocab_ref, out_ref):
        for at in range(0, width, 512):
            out_ref[:, at : at + 512] = lax.dot_general(
                grads_ref[...],
                vocab_ref[at : at + 512],
                (((1,), (1,)), ((), ())),
                preferred_element_type=F32,
            ).astype(BF16)

    return call(
        kernel,
        (1,),
        [NEAR, NEAR],
        NEAR,
        pltpu.VMEM((tokens, width), BF16),
        [grads, vocab],
        2 * tokens * columns * width,
    )


def shards(
    hidden_act,
    down_weight,
    residual,
    post_gain,
    final_gain,
    vocab,
    vocab_bias,
    target_ids,
    target_weights,
):
    own_rows = residual.shape[0]
    width, columns = vocab.shape
    vp_index = lax.axis_index(VP)
    z_index = lax.axis_index("z")
    core = lax.axis_index("c")
    n_z = lax.axis_size("z")

    branch_parts = jnp.dot(hidden_act, down_weight, preferred_element_type=F32).astype(BF16)
    branch = summed_over(branch_parts, VP)
    stream = residual.astype(F32) + branch * inverse_rms(branch) * post_gain
    inverse = inverse_rms(stream)
    normed = (stream * inverse * final_gain).astype(BF16)

    gathered = copied_over(normed, VP)
    ids = target_ids - vp_index * columns
    chunk = width // n_z
    far = n_z // 2
    way = 1 - 2 * core
    index = jnp.stack(
        [1 - core]
        + [(z_index + way * d + n_z) % n_z for d in range(far + 1)]
        + [(z_index - way * d + n_z) % n_z for d in range(far + 1)]
    )

    wanted = wanted_matrix(ids, target_weights, columns, (branch_parts, index))
    scores, stats, near_vocab, near_wanted, normed_rows = scored(
        gathered, vocab, vocab_bias, wanted
    )
    n_vp = lax.axis_size(VP)
    stats = exchange(jnp.broadcast_to(stats, (n_vp, *stats.shape)), VP)
    row_max = jnp.max(stats[:, 0], axis=0)
    row_sum = jnp.sum(stats[:, 1] * jnp.exp(stats[:, 0] - row_max), axis=0)
    target_score = jnp.sum(stats[:, 2], axis=0)
    log_norm = row_max + jnp.log(row_sum)
    group_losses = log_norm - target_score + z_weight * log_norm * log_norm
    losses = lax.dynamic_slice_in_dim(group_losses, vp_index * own_rows, own_rows)

    def swapped(x):
        return lax.ppermute(x, "c", [(0, 1), (1, 0)])

    ring = [
        (z * 2 + c, (z + (1, -1)[c]) % n_z * 2 + c) for z in range(n_z) for c in (0, 1)
    ]

    def sent(x):
        return lax.ppermute(x.astype(BF16), DP, ring)

    def own_block(distance, lane):
        return (1 + distance, 1 - lane)

    def their_block(distance, lane):
        return (2 + far + distance, lane)

    first = [(far, 0), (far - 1, 1), (far - 1, 0)]
    rest = [(d, lane) for d in range(far - 2, 0, -1) for lane in (1, 0)]
    owned = first + rest + [(0, 0), (0, 1)]
    grads, products = gradients(
        scores,
        log_norm,
        near_wanted,
        normed_rows,
        index,
        [[their_block(*key) for key in first]]
        + [[their_block(*key)] for key in rest]
        + [[own_block(*key)] for key in owned],
        chunk,
    )
    passed_first = swapped(products[0])
    passed = {key: passed_first[at] for at, key in enumerate(first)}
    passed.update({key: swapped(block)[0] for key, block in zip(rest, products[1:])})
    own = {key: block[0] for key, block in zip(owned, products[1 + len(rest) :])}

    def message(key, *carried):
        return sum(x.astype(F32) for x in (own[key], passed[key], *carried)).astype(BF16)

    carried = [sent(message((far, 0))), sent(message((far - 1, 1)))]
    for distance in range(far - 1, 0, -1):
        for lane, key in ((0, (distance, 0)), (1, (distance - 1, 1))):
            if key in owned and key[0] > 0:
                carried[lane] = sent(message(key, carried[lane]))
    slice_rows = chunk // 2
    arrived, passed = [], []
    for lane in (0, 1):
        for side, parts in ((core, arrived), (1 - core, passed)):
            parts.append(
                sum(
                    lax.dynamic_slice_in_dim(x, side * slice_rows, slice_rows).astype(F32)
                    for x in (own[0, lane], carried[lane])
                )
            )
        passed[lane] = swapped(passed[lane].astype(BF16)).astype(F32)
    lanes = [arrived[0] + passed[1], arrived[1] + passed[0]]
    vocab_grad = jnp.concatenate(
        [jnp.where(core == 0, lanes[0], lanes[1]), jnp.where(core == 0, lanes[1], lanes[0])], axis=1
    )

    row_parts = row_gradients(grads, near_vocab)
    row_grad = summed_over(row_parts, VP)
    upstream = row_grad * final_gain
    stream_grad = inverse * (
        upstream - stream * inverse * inverse * jnp.mean(upstream * stream, axis=-1, keepdims=True)
    )
    return (losses, stream_grad, vocab_grad)


def solution(mesh):
    split = Mesh(mesh.devices.reshape(4, 4, mesh.shape["dp"] // 2, 2), ("y", "x", "z", "c"))
    placed = (
        P(DP, VP),
        P(VP, None),
        P(DP_VP, None),
        P(),
        P(),
        P(None, VP),
        P(VP),
        P(DP, None),
        P(DP, None),
    )

    return jax.shard_map(
        shards,
        mesh=split,
        in_specs=placed,
        out_specs=(P(DP_VP), P(DP_VP, None), P(DP, VP)),
        check_vma=False,
    )
```

```python
import jax
import jax.numpy as jnp
from jax import lax
from jax.experimental import pallas as pl
from jax.experimental.pallas import tpu as pltpu
from jax.sharding import Mesh
from jax.sharding import PartitionSpec as P


F32 = jnp.float32
BF16 = jnp.bfloat16
VP = ("y", "x")
DP = ("z", "c")
DP_VP = ("z", "c", "y", "x")

epsilon = 1e-06
z_weight = 0.001
loss_scale = 32.0


def exchange(parts, axis):
    return lax.all_to_all(parts, axis, split_axis=0, concat_axis=0, tiled=True)


def summed_over(rows, axis):
    size = lax.axis_size(axis)
    parts = rows.astype(BF16).reshape(size, rows.shape[0] // size, rows.shape[1])
    return jnp.sum(exchange(parts, axis).astype(F32), axis=0)


def copied_over(rows, axis):
    size = lax.axis_size(axis)
    copies = jnp.broadcast_to(rows, (size, *rows.shape))
    return exchange(copies, axis).reshape(size * rows.shape[0], rows.shape[1])


def inverse_rms(values):
    return lax.rsqrt(jnp.mean(values * values, axis=-1, keepdims=True) + epsilon)


def call(kernel, grid, in_specs, out_specs, out_shape, operands, flops, after=(), scratch=(), scalars=None, aliases={}, vmem=16):
    lead = 0 if scalars is None else 1
    used = len(operands)

    def body(*refs):
        kernel(*refs[: lead + used], *refs[lead + used + len(after) :])

    moved = sum(x.size * x.dtype.itemsize for x in operands)
    return pl.pallas_call(
        body,
        grid_spec=pltpu.PrefetchScalarGridSpec(
            num_scalar_prefetch=lead,
            grid=grid,
            in_specs=list(in_specs) + [pl.BlockSpec(memory_space=pl.ANY)] * len(after),
            out_specs=out_specs,
            scratch_shapes=scratch,
        ),
        out_shape=out_shape,
        input_output_aliases=aliases,
        compiler_params=pltpu.CompilerParams(vmem_limit_bytes=vmem << 20),
        cost_estimate=pl.CostEstimate(flops=flops, bytes_accessed=moved, transcendentals=0),
    )(*(() if scalars is None else (scalars,)), *operands, *after)


LANES = 128
SCORE_BLOCK = 512
HBM = pl.BlockSpec(memory_space=pltpu.HBM)
NEAR = pl.BlockSpec(memory_space=pltpu.VMEM)


def wanted_matrix(ids, weights, columns, after):
    tokens = ids.shape[0]
    rows = 128

    def kernel(ids_ref, weights_ref, out_ref):
        wide = (rows, LANES)
        at_ids = [jnp.broadcast_to(ids_ref[:, k : k + 1], wide) for k in range(ids.shape[1])]
        at_weights = [jnp.broadcast_to(weights_ref[:, k : k + 1], wide) for k in range(ids.shape[1])]
        lane = lax.broadcasted_iota(jnp.int32, wide, 1)
        for at in range(0, columns, LANES):
            found = jnp.zeros(wide, F32)
            for k in range(ids.shape[1]):
                found = found + jnp.where(at_ids[k] == lane + at, at_weights[k], 0.0)
            out_ref[:, at : at + LANES] = found

    def block(shape):
        return pl.BlockSpec((rows, shape[1]), lambda i: (i, 0))

    return call(
        kernel,
        (tokens // rows,),
        [block(ids.shape), block(weights.shape)],
        block((tokens, columns)),
        jax.ShapeDtypeStruct((tokens, columns), F32),
        [ids, weights],
        8 * tokens * columns,
        after,
    )


def scored(rows, vocab, bias, wanted):
    tokens, width = rows.shape
    columns = vocab.shape[1]
    blocks = [slice(at, at + SCORE_BLOCK) for at in range(0, columns, SCORE_BLOCK)]

    def kernel(rows_ref, vocab_hbm, bias_ref, wanted_hbm, out_ref, stats_ref, wanted_ref, turned_ref, vocab_ref, sems):
        deep = width // 4
        load_vocab = [
            pltpu.make_async_copy(
                vocab_hbm.at[pl.ds(i * deep, deep)], vocab_ref.at[pl.ds(i * deep, deep)], sems.at[i]
            )
            for i in range(4)
        ]
        load_wanted = pltpu.make_async_copy(wanted_hbm, wanted_ref, sems.at[4])
        near, rest = slice(0, 2 * deep), slice(2 * deep, width)
        load_vocab[0].start()
        load_vocab[1].start()
        load_vocab[0].wait()
        load_vocab[2].start()
        load_vocab[1].wait()
        load_vocab[3].start()
        load_wanted.start()
        turn = width // len(blocks)
        for j, across in enumerate(blocks):
            out_ref[:, across] = jnp.dot(
                rows_ref[:, near], vocab_ref[near, across], preferred_element_type=F32
            )
            turned_ref[j * turn : (j + 1) * turn] = rows_ref[:, j * turn : (j + 1) * turn].T
        top = jnp.full((tokens, LANES), -jnp.inf, F32)
        total = jnp.zeros((tokens, LANES), F32)
        target = jnp.zeros((tokens, LANES), F32)
        load_vocab[2].wait()
        load_vocab[3].wait()
        load_wanted.wait()
        for j in range(len(blocks) + 1):
            if j < len(blocks):
                across = blocks[j]
                out_ref[:, across] = (
                    out_ref[:, across]
                    + jnp.dot(rows_ref[:, rest], vocab_ref[rest, across], preferred_element_type=F32)
                    + bias_ref[:, across]
                )
            if j > 0:
                across = blocks[j - 1]
                lanes = [slice(at, at + LANES) for at in range(across.start, across.stop, LANES)]
                new_top = top
                for at in lanes:
                    new_top = jnp.maximum(new_top, out_ref[:, at])
                total = total * jnp.exp(top - new_top)
                for at in lanes:
                    part = out_ref[:, at]
                    total = total + jnp.exp(part - new_top)
                    target = target + wanted_ref[:, at] * part
                top = new_top
        row_top = jnp.max(top, axis=1, keepdims=True)
        row_total = jnp.sum(total * jnp.exp(top - row_top), axis=1, keepdims=True)
        row_target = jnp.sum(target, axis=1, keepdims=True)
        lane = lax.broadcasted_iota(jnp.int32, (tokens, LANES), 1)
        packed = jnp.where(lane == 0, row_top, jnp.where(lane == 1, row_total, row_target))
        stats_ref[...] = packed.T[:8]

    scores, stats, near_wanted, turned = call(
        kernel,
        (1,),
        [NEAR, HBM, pl.BlockSpec((1, columns), lambda i: (0, 0)), HBM],
        [NEAR, pl.BlockSpec((8, tokens), lambda i: (0, 0)), NEAR, NEAR],
        [
            pltpu.VMEM((tokens, columns), F32),
            jax.ShapeDtypeStruct((8, tokens), F32),
            pltpu.VMEM(wanted.shape, wanted.dtype),
            pltpu.VMEM((width, tokens), rows.dtype),
        ],
        [rows, vocab, bias.reshape(1, columns), wanted],
        2 * tokens * width * columns,
        scratch=[pltpu.VMEM(vocab.shape, vocab.dtype), pltpu.SemaphoreType.DMA((5,))],
        vmem=50,
    )
    return scores, stats[:3], near_wanted, turned


def multiply_blocks(index_ref, rows_ref, kept_ref, outs, lists, chunk):
    for out, some in zip(outs, lists):
        for k, (place, slot) in enumerate(some):
            side = index_ref[0] if slot == 0 else 1 - index_ref[0]
            start = pl.multiple_of(index_ref[place] * chunk, chunk)
            out[k] = jnp.dot(
                rows_ref[pl.ds(start, chunk)], kept_ref[side], preferred_element_type=F32
            ).astype(BF16)


def gradients(scores, log_norm, wanted, rows, index, lists, chunk):
    tokens, columns = scores.shape
    half = columns // 2
    part = 128

    def kernel(index_ref, scores_ref, norm_ref, wanted_ref, rows_ref, grads_ref, kept_ref, *outs):
        norms = jnp.broadcast_to(norm_ref[...], (LANES, tokens)).T
        for i in range(0, tokens, part):
            norm = norms[i : i + part]
            factor = 1.0 + 2.0 * z_weight * norm
            for at in range(0, columns, LANES):
                cell = (slice(i, i + part), slice(at, at + LANES))
                probability = jnp.exp(scores_ref[cell] - norm)
                value = (loss_scale * (probability * factor - wanted_ref[cell])).astype(BF16)
                grads_ref[cell] = value
                kept_ref[at // half, cell[0], at % half : at % half + LANES] = value
        multiply_blocks(index_ref, rows_ref, kept_ref, outs, lists, chunk)

    results = call(
        kernel,
        (1,),
        [NEAR, pl.BlockSpec((1, tokens), lambda i, idx: (0, 0)), NEAR, NEAR],
        [NEAR] * (2 + len(lists)),
        [pltpu.VMEM(scores.shape, BF16), pltpu.VMEM((2, tokens, half), BF16)]
        + [pltpu.VMEM((len(some), chunk, half), BF16) for some in lists],
        [scores, log_norm[None], wanted, rows],
        2 * chunk * half * tokens * sum(len(some) for some in lists),
        scalars=index,
    )
    return results[0], results[1], results[2:]


def block_products(rows, kept, index, lists, chunk):
    tokens = rows.shape[1]
    half = kept.shape[2]

    def kernel(index_ref, rows_ref, kept_ref, *outs):
        multiply_blocks(index_ref, rows_ref, kept_ref, outs, lists, chunk)

    return call(
        kernel,
        (1,),
        [NEAR, NEAR],
        [NEAR] * len(lists),
        [pltpu.VMEM((len(some), chunk, half), BF16) for some in lists],
        [rows, kept],
        2 * chunk * half * tokens * sum(len(some) for some in lists),
        scalars=index,
    )


def row_gradients(grads, vocab):
    tokens, columns = grads.shape
    width = vocab.shape[0]

    def kernel(grads_ref, vocab_ref, out_ref):
        for at in range(0, width, 512):
            out_ref[:, at : at + 512] = lax.dot_general(
                grads_ref[...],
                vocab_ref[at : at + 512],
                (((1,), (1,)), ((), ())),
                preferred_element_type=F32,
            ).astype(BF16)

    return call(
        kernel,
        (1,),
        [NEAR, NEAR],
        NEAR,
        pltpu.VMEM((tokens, width), BF16),
        [grads, vocab],
        2 * tokens * columns * width,
    )


def shards(
    hidden_act,
    down_weight,
    residual,
    post_gain,
    final_gain,
    vocab,
    vocab_bias,
    target_ids,
    target_weights,
):
    own_rows = residual.shape[0]
    width, columns = vocab.shape
    vp_index = lax.axis_index(VP)
    z_index = lax.axis_index("z")
    core = lax.axis_index("c")
    n_z = lax.axis_size("z")

    branch_parts = jnp.dot(hidden_act, down_weight, preferred_element_type=F32).astype(BF16)
    branch = summed_over(branch_parts, VP)
    stream = residual.astype(F32) + branch * inverse_rms(branch) * post_gain
    inverse = inverse_rms(stream)
    normed = (stream * inverse * final_gain).astype(BF16)

    gathered = copied_over(normed, VP)
    ids = target_ids - vp_index * columns
    chunk = width // n_z
    far = n_z // 2
    way = 1 - 2 * core
    index = jnp.stack(
        [1 - core]
        + [(z_index + way * d + n_z) % n_z for d in range(far + 1)]
        + [(z_index - way * d + n_z) % n_z for d in range(far + 1)]
    )

    wanted = wanted_matrix(ids, target_weights, columns, (branch_parts, index))
    scores, stats, near_wanted, normed_rows = scored(
        gathered, vocab, vocab_bias, wanted
    )
    n_vp = lax.axis_size(VP)
    stats = exchange(jnp.broadcast_to(stats, (n_vp, *stats.shape)), VP)
    row_max = jnp.max(stats[:, 0], axis=0)
    row_sum = jnp.sum(stats[:, 1] * jnp.exp(stats[:, 0] - row_max), axis=0)
    target_score = jnp.sum(stats[:, 2], axis=0)
    log_norm = row_max + jnp.log(row_sum)
    group_losses = log_norm - target_score + z_weight * log_norm * log_norm
    losses = lax.dynamic_slice_in_dim(group_losses, vp_index * own_rows, own_rows)

    def swapped(x):
        return lax.ppermute(x, "c", [(0, 1), (1, 0)])

    ring = [
        (z * 2 + c, (z + (1, -1)[c]) % n_z * 2 + c) for z in range(n_z) for c in (0, 1)
    ]

    def sent(x):
        return lax.ppermute(x.astype(BF16), DP, ring)

    def own_block(distance, lane):
        return (1 + distance, 1 - lane)

    def their_block(distance, lane):
        return (2 + far + distance, lane)

    first = [(far, 0), (far - 1, 1), (far - 1, 0)]
    rest = [(d, lane) for d in range(far - 2, 0, -1) for lane in (1, 0)]
    owned = first + rest + [(0, 0), (0, 1)]
    grads, kept, (theirs_first,) = gradients(
        scores,
        log_norm,
        near_wanted,
        normed_rows,
        index,
        [[their_block(*key) for key in first]],
        chunk,
    )
    passed_first = swapped(theirs_first)
    products = block_products(
        normed_rows,
        kept,
        index,
        [[own_block(*key)] for key in owned] + [[their_block(*key)] for key in rest],
        chunk,
    )
    passed = {key: passed_first[at] for at, key in enumerate(first)}
    passed.update({key: swapped(block)[0] for key, block in zip(rest, products[len(owned) :])})
    own = {key: block[0] for key, block in zip(owned, products)}

    def message(key, *carried):
        return sum(x.astype(F32) for x in (own[key], passed[key], *carried)).astype(BF16)

    carried = [sent(message((far, 0))), sent(message((far - 1, 1)))]
    for distance in range(far - 1, 0, -1):
        for lane, key in ((0, (distance, 0)), (1, (distance - 1, 1))):
            if key in owned and key[0] > 0:
                carried[lane] = sent(message(key, carried[lane]))
    slice_rows = chunk // 2
    arrived, passed = [], []
    for lane in (0, 1):
        for side, parts in ((core, arrived), (1 - core, passed)):
            parts.append(
                sum(
                    lax.dynamic_slice_in_dim(x, side * slice_rows, slice_rows).astype(F32)
                    for x in (own[0, lane], carried[lane])
                )
            )
        passed[lane] = swapped(passed[lane].astype(BF16)).astype(F32)
    lanes = [arrived[0] + passed[1], arrived[1] + passed[0]]
    vocab_grad = jnp.concatenate(
        [jnp.where(core == 0, lanes[0], lanes[1]), jnp.where(core == 0, lanes[1], lanes[0])], axis=1
    )

    row_parts = row_gradients(grads, vocab)
    row_grad = summed_over(row_parts, VP)
    upstream = row_grad * final_gain
    stream_grad = inverse * (
        upstream - stream * inverse * inverse * jnp.mean(upstream * stream, axis=-1, keepdims=True)
    )
    return (losses, stream_grad, vocab_grad)


def solution(mesh):
    split = Mesh(mesh.devices.reshape(4, 4, mesh.shape["dp"] // 2, 2), ("y", "x", "z", "c"))
    placed = (
        P(DP, VP),
        P(VP, None),
        P(DP_VP, None),
        P(),
        P(),
        P(None, VP),
        P(VP),
        P(DP, None),
        P(DP, None),
    )

    return jax.shard_map(
        shards,
        mesh=split,
        in_specs=placed,
        out_specs=(P(DP_VP), P(DP_VP, None), P(DP, VP)),
        check_vma=False,
    )
```
